32 devices in a mesh: fs: 8 (over z, y), tp: 4 (over x, core).
Axes of the slice: x: 2, y: 2, z: 4, core: 2. Of those that a mesh axis runs over, the one named last changes fastest.
Arguments:
- tokens: bfloat16 [8192, 2048], P('fs'), may hold values from -6 to 6
- w_gate_side: bfloat16 [2048, 1024], P('fs', 'tp'), may hold values from -0.125 to 0.125
- w_value_side: bfloat16 [2048, 1024], P('fs', 'tp'), may hold values from -0.125 to 0.125
- spatial_gain: float32 [1024], P('tp'), may hold values from 0.1 to 1.9
- w_spatial: bfloat16 [16, 128, 128], P('tp'), may hold values from -0.5 to 0.5
- spatial_bias: float32 [16, 128], P('tp'), may hold values from 0.1 to 1.9
- w_mixer_out: bfloat16 [1024, 2048], P('tp', 'fs'), may hold values from -0.1875 to 0.1875
- first_gain: float32 [2048], replicated, may hold values from 0.1 to 1.9
- w_ff_gate: bfloat16 [2048, 5632], P('fs', 'tp'), may hold values from -0.125 to 0.125
- w_ff_up: bfloat16 [2048, 5632], P('fs', 'tp'), may hold values from -0.125 to 0.125
- conv_gate_taps: float32 [3, 5632], P(None, 'tp'), may hold values from -3.5 to 3.5
- conv_up_taps: float32 [3, 5632], P(None, 'tp'), may hold values from -3.5 to 3.5
- w_ff_down: bfloat16 [5632, 2048], P('tp', 'fs'), may hold values from -0.078125 to 0.078125
- second_gain: float32 [2048], replicated, may hold values from 0.1 to 1.9
Outputs:
- layer_out: bfloat16 [8192, 2048], P('fs', 'tp')
The draws below stay inside these ranges and needn't reach their ends.
All inputs are finite; a program needn't handle non-finite values.
Results may differ from the reference program's by a relative error of at most 0.015.
Values may be sent and summed in bfloat16 or wider, within the bound.
No kernel may reach another device: no remote copies, remote signals or barrier semaphores. Data moves between devices by JAX's collectives and lax.ppermute only.
A program may use at most 64 MiB of HBM per device.

```python
import jax
import jax.numpy as jnp
from jax import lax

D = 2048
GROUPS = 16
GROUP_DIM = 64
SG_WIDTH = 1024
FF = 5632
SPAN = 128
SEQ = 256
TOKENS = 8192
N_TP = 4


def steps_of(stream_key, shape, split, least, high):
    def one(axis_at, blocks):
        steps = jax.random.uniform(jax.random.fold_in(jax.random.fold_in(stream_key, 6), axis_at), (blocks,), jnp.float32, least / len(split), high / len(split))
        return jnp.repeat(jnp.exp(steps), shape[axis_at] // blocks).reshape((-1,) + (1,) * (len(shape) - axis_at - 1))

    level = one(*split[0])
    for cut in split[1:]:
        level = level * one(*cut)
    return level


def noise(key, shape, scale, limit, shards=(), kind=jnp.bfloat16):
    level = steps_of(key, shape, shards, -0.22, 0.18) if shards else 1.0
    values = jax.random.normal(key, shape, jnp.float32) * scale * level
    return jnp.minimum(jnp.maximum(values, -limit), limit).astype(kind)


def setup_inputs(seed: int = 0) -> dict:
    key_of = jax.random.split(jax.random.key(seed), 15)
    tokens = noise(key_of[0], (TOKENS, D), 1.0, 6.0, ((0, 8),))
    w_gate_side = noise(key_of[1], (D, SG_WIDTH), D ** -0.5, 0.125, ((0, 8), (1, 4)))
    w_value_side = noise(key_of[2], (D, SG_WIDTH), D ** -0.5, 0.125, ((0, 8), (1, 4)))
    spatial_gain = jnp.clip(1.0 + 0.18 * jax.random.normal(key_of[3], (SG_WIDTH,), jnp.float32), 0.1, 1.9)
    w_spatial = noise(key_of[4], (GROUPS, SPAN, SPAN), SPAN ** -0.5, 0.5, ((0, 4),))
    spatial_bias = jnp.clip(1.0 + 0.18 * jax.random.normal(key_of[5], (GROUPS, SPAN), jnp.float32), 0.1, 1.9)
    w_mixer_out = noise(key_of[6], (SG_WIDTH, D), SG_WIDTH ** -0.5, 0.1875, ((0, 4), (1, 8)))
    first_gain = jnp.clip(1.0 + 0.18 * jax.random.normal(key_of[7], (D,), jnp.float32), 0.1, 1.9)
    w_ff_gate = noise(key_of[8], (D, FF), D ** -0.5, 0.125, ((0, 8), (1, 4)))
    w_ff_up = noise(key_of[9], (D, FF), D ** -0.5, 0.125, ((0, 8), (1, 4)))
    conv_gate_taps = noise(key_of[10], (3, FF), 3 ** -0.5, 3.5, ((1, 4),), jnp.float32)
    conv_up_taps = noise(key_of[11], (3, FF), 3 ** -0.5, 3.5, ((1, 4),), jnp.float32)
    w_ff_down = noise(key_of[12], (FF, D), FF ** -0.5, 0.078125, ((0, 4), (1, 8)))
    second_gain = jnp.clip(1.0 + 0.18 * jax.random.normal(key_of[13], (D,), jnp.float32), 0.1, 1.9)
    return {"tokens": tokens, "w_gate_side": w_gate_side, "w_value_side": w_value_side, "spatial_gain": spatial_gain, "w_spatial": w_spatial, "spatial_bias": spatial_bias, "w_mixer_out": w_mixer_out, "first_gain": first_gain, "w_ff_gate": w_ff_gate, "w_ff_up": w_ff_up, "conv_gate_taps": conv_gate_taps, "conv_up_taps": conv_up_taps, "w_ff_down": w_ff_down, "second_gain": second_gain}


residual_scale = 2.0 ** 0.25
norm_eps = 1e-05

def row_norm(values, gain):
    width = values.shape[-1]
    mean = lax.optimization_barrier(jnp.sum(values, axis=-1, keepdims=True)) / width
    square = lax.optimization_barrier(jnp.sum(values * values, axis=-1, keepdims=True)) / width
    spread = square - mean * mean
    return (values - mean) * lax.rsqrt(spread + norm_eps) * gain

def causal_taps(pre, taps):
    count = pre.shape[0] // SEQ
    blocks = pre.reshape(count, SEQ, pre.shape[1])
    padded = jnp.pad(blocks, ((0, 0), (2, 0), (0, 0)))
    result = padded[:, 0:SEQ] * taps[0] + padded[:, 1:SEQ + 1] * taps[1] + padded[:, 2:] * taps[2]
    return result.reshape(pre.shape)

def range_sum(left, right, parts):
    width = left.shape[1] // parts
    total = jnp.zeros((left.shape[0], right.shape[1]), jnp.float32)
    for index in range(parts):
        term = jnp.dot(left[:, index * width:(index + 1) * width], right[index * width:(index + 1) * width], preferred_element_type=jnp.float32)
        total = total + term.astype(jnp.bfloat16).astype(jnp.float32)
    return total

def reference(tokens, w_gate_side, w_value_side, spatial_gain, w_spatial, spatial_bias, w_mixer_out, first_gain, w_ff_gate, w_ff_up, conv_gate_taps, conv_up_taps, w_ff_down, second_gain):
    gate_act = jax.nn.gelu(jnp.dot(tokens, w_gate_side, preferred_element_type=jnp.float32))
    value_act = jax.nn.gelu(jnp.dot(tokens, w_value_side, preferred_element_type=jnp.float32))
    value_norm = row_norm(value_act, spatial_gain).astype(jnp.bfloat16)
    blocks = value_norm.reshape(TOKENS // SPAN, SPAN, GROUPS, GROUP_DIM).astype(jnp.float32)
    lower = jnp.tril(jnp.ones((SPAN, SPAN), jnp.float32))
    causal_w = w_spatial.astype(jnp.float32) * lower
    mixed = jnp.einsum('gts,nsgc->ntgc', causal_w, blocks) + spatial_bias.T[None, :, :, None]
    spatial_out = (gate_act * mixed.reshape(TOKENS, SG_WIDTH)).astype(jnp.bfloat16)
    mixer_sum = range_sum(spatial_out, w_mixer_out, N_TP)
    first_normed = row_norm(residual_scale * tokens.astype(jnp.float32) + mixer_sum, first_gain).astype(jnp.bfloat16)
    ff_gate = causal_taps(jnp.dot(first_normed, w_ff_gate, preferred_element_type=jnp.float32), conv_gate_taps)
    ff_up = causal_taps(jnp.dot(first_normed, w_ff_up, preferred_element_type=jnp.float32), conv_up_taps)
    ff_hidden = (jax.nn.silu(ff_gate) * ff_up).astype(jnp.bfloat16)
    ff_sum = range_sum(ff_hidden, w_ff_down, N_TP)
    layer_out = row_norm(residual_scale * first_normed.astype(jnp.float32) + ff_sum, second_gain)
    return layer_out.astype(jnp.bfloat16)
```

```python
import jax
import jax.numpy as jnp
import numpy as np
from jax import lax
from jax.experimental import pallas as pl
from jax.experimental.pallas import tpu as pltpu
from jax.sharding import PartitionSpec as P

SPAN = 128
SEQ = 256

residual_scale = 2.0**0.25
norm_eps = 1e-05


BF = jnp.bfloat16
F32 = jnp.float32


def cycle_of(mesh):
    spots = [d.coords for d in mesh.devices[:, 0]]
    at = {(c[2], c[1]): i for i, c in enumerate(spots)}
    zs = sorted({p[0] for p in at})
    ys = sorted({p[1] for p in at})
    walk = []
    for i, z in enumerate(zs):
        walk += [at[(z, y)] for y in (ys[1:] if i % 2 == 0 else ys[:0:-1])]
    return walk + [at[(z, ys[0])] for z in reversed(zs)]


class Ring:
    def __init__(self, walk):
        self.walk = walk
        n = len(walk)
        self.n = n
        self.fwd = [(walk[i], walk[(i + 1) % n]) for i in range(n)]
        self.bwd = [(walk[i], walk[(i - 1) % n]) for i in range(n)]
        offsets = [0]
        for s in range(1, n // 2):
            offsets += [-s, s]
        offsets += [n // 2]
        table = np.zeros((n, n), np.int32)
        for r, dev in enumerate(walk):
            table[dev] = [walk[(r + o) % n] for o in offsets]
        self.table = table

    def index(self):
        row = lax.dynamic_slice_in_dim(jnp.asarray(self.table), lax.axis_index("fs"), 1, 0)
        return row[0]

    def gather(self, w):
        half = w.shape[0] // 2
        out = [w]
        a = b = w
        for _ in range(self.n // 2 - 1):
            a = lax.ppermute(a, "fs", self.fwd)
            b = lax.ppermute(b, "fs", self.bwd)
            out += [a, b]
        out += [lax.ppermute(a[:half], "fs", self.fwd), lax.ppermute(b[half:], "fs", self.bwd)]
        return out


def copies(chunks, place, sem):
    n = len(chunks) - 1
    todo = [pltpu.make_async_copy(chunks[k], place(k, None), sem) for k in range(n - 1)]
    todo += [pltpu.make_async_copy(chunks[n - 1 + h], place(n - 1, h), sem) for h in range(2)]
    return todo


def any_specs(count):
    return [pl.BlockSpec(memory_space=pl.ANY)] * count


def smem_spec():
    return pl.BlockSpec(memory_space=pltpu.SMEM)


def tiles_of(width, step):
    return [(at, min(step, width - at)) for at in range(0, width, step)]


def row_place(idx, ref, rows):
    def place(k, half):
        size = rows if half is None else rows // 2
        start = idx[k] * rows + (0 if half is None else half * size)
        return ref.at[pl.ds(pl.multiple_of(start, size), size), :]

    return place


def col_place(idx, ref, cols):
    def place(k, half):
        lanes = pl.ds(pl.multiple_of(idx[k] * cols, cols), cols)
        if half is None:
            return ref.at[:, lanes]
        size = ref.shape[0] // 2
        return ref.at[pl.ds(half * size, size), lanes]

    return place


def gate_value(idx, tokens, chunks, width):
    rows, dim = tokens.shape
    part = chunks[0].shape[0]
    tile = 256

    def body(idx_ref, x_ref, *rest):
        refs, (gate_ref, value_ref), (w_ref, sem) = rest[: len(chunks)], rest[len(chunks) : -2], rest[-2:]

        @pl.when(pl.program_id(0) == 0)
        def _():
            sources = [r.at[:, pl.ds(0, 2 * width)] for r in refs]
            todo = copies(sources, row_place(idx_ref, w_ref, part), sem)
            for c in todo:
                c.start()
            for c in todo:
                c.wait()

        pre = jnp.dot(x_ref[...], w_ref[...], preferred_element_type=F32)
        act = jax.nn.gelu(pre)
        value_ref[...] = act[:, :width]
        gate_ref[...] = act[:, width:]

    return pl.pallas_call(
        body,
        grid=(rows // tile,),
        in_specs=[smem_spec(), pl.BlockSpec((tile, dim), lambda i: (i, 0))] + any_specs(len(chunks)),
        out_specs=[pl.BlockSpec((tile, width), lambda i: (i, 0))] * 2,
        out_shape=[jax.ShapeDtypeStruct((rows, width), F32)] * 2,
        scratch_shapes=[pltpu.VMEM((dim, 2 * width), BF), pltpu.SemaphoreType.DMA],
        compiler_params=pltpu.CompilerParams(dimension_semantics=("arbitrary",)),
        name="gate_value",
    )(idx, tokens, *chunks)


def mixer(idx, gate_act, value_act, shift, scale, gain, w_spatial, bias_t, chunks, dim):
    rows, width = gate_act.shape
    groups = w_spatial.shape[0]
    lanes = width // groups
    cols = dim // (len(chunks) - 1)

    def body(idx_ref, gate_ref, value_ref, shift_ref, scale_ref, gain_ref, ws_ref, bias_ref, *rest):
        refs, out_ref, (w_ref, sem) = rest[: len(chunks)], rest[len(chunks)], rest[-2:]
        first = pl.program_id(0) == 0

        def todo():
            return copies(list(refs), col_place(idx_ref, w_ref, cols), sem)

        @pl.when(first)
        def _():
            for c in todo():
                c.start()

        normed = (value_ref[...] - shift_ref[...]) * scale_ref[...] * gain_ref[...]
        normed = normed.astype(BF)
        lower = lax.broadcasted_iota(jnp.int32, (SPAN, SPAN), 0) >= lax.broadcasted_iota(
            jnp.int32, (SPAN, SPAN), 1
        )
        group_of = lax.broadcasted_iota(jnp.int32, (SPAN, width), 1) // lanes
        mixed = jnp.zeros((SPAN, width), F32)
        for g in range(groups):
            w = jnp.where(lower, ws_ref[g].astype(F32), 0.0).astype(BF)
            term = jnp.dot(w, normed, preferred_element_type=F32) + bias_ref[:, g : g + 1]
            mixed = jnp.where(group_of == g, term, mixed)
        spatial = (gate_ref[...] * mixed).astype(BF)

        @pl.when(first)
        def _():
            for c in todo():
                c.wait()

        out_ref[...] = jnp.dot(spatial, w_ref[...], preferred_element_type=F32).astype(BF)

    whole = lambda shape: pl.BlockSpec(shape, lambda i: (0,) * len(shape))
    return pl.pallas_call(
        body,
        grid=(rows // SPAN,),
        in_specs=[
            smem_spec(),
            pl.BlockSpec((SPAN, width), lambda i: (i, 0)),
            pl.BlockSpec((SPAN, width), lambda i: (i, 0)),
            pl.BlockSpec((SPAN, 1), lambda i: (i, 0)),
            pl.BlockSpec((SPAN, 1), lambda i: (i, 0)),
            whole((1, width)),
            whole(w_spatial.shape),
            whole((SPAN, groups)),
        ]
        + any_specs(len(chunks)),
        out_specs=pl.BlockSpec((SPAN, dim), lambda i: (i, 0)),
        out_shape=jax.ShapeDtypeStruct((rows, dim), BF),
        scratch_shapes=[pltpu.VMEM((width, dim), BF), pltpu.SemaphoreType.DMA],
        compiler_params=pltpu.CompilerParams(dimension_semantics=("arbitrary",)),
        name="mixer",
    )(idx, gate_act, value_act, shift, scale, gain, w_spatial, bias_t, *chunks)


def taps_of(pre, taps):
    row = lax.broadcasted_iota(jnp.int32, pre.shape, 0)
    one = jnp.where(row >= 1, pltpu.roll(pre, 1, 0), 0.0)
    two = jnp.where(row >= 2, pltpu.roll(pre, 2, 0), 0.0)
    return two * taps[0:1] + one * taps[1:2] + pre * taps[2:3]


def feed_forward(idx, own_at, tokens, mixer_sum, gain, gate_chunks, up_chunks, gate_taps, up_taps, own):
    rows, dim = tokens.shape
    part, width = gate_chunks[0].shape
    n = len(gate_chunks)

    def body(idx_ref, at_ref, x_ref, m_ref, gain_ref, gt_ref, ut_ref, *rest):
        gates, ups, (hid_ref, own_ref) = rest[:n], rest[n : 2 * n], rest[2 * n : 2 * n + 2]
        wg_ref, wu_ref, norm_ref, sems = rest[2 * n + 2 :]
        first = pl.program_id(0) == 0

        def todo():
            return copies(list(gates), row_place(idx_ref, wg_ref, part), sems.at[0]) + copies(
                list(ups), row_place(idx_ref, wu_ref, part), sems.at[1]
            )

        @pl.when(first)
        def _():
            for c in todo():
                c.start()

        x = residual_scale * x_ref[...].astype(F32) + m_ref[...].astype(F32)
        mean = jnp.sum(x, axis=1, keepdims=True) / dim
        spread = jnp.sum(x * x, axis=1, keepdims=True) / dim - mean * mean
        norm_ref[...] = ((x - mean) * lax.rsqrt(spread + norm_eps) * gain_ref[...]).astype(BF)
        own_ref[...] = norm_ref[:, pl.ds(pl.multiple_of(at_ref[0], own), own)]

        @pl.when(first)
        def _():
            for c in todo():
                c.wait()

        for at, size in tiles_of(width, 256):
            here = pl.ds(at, size)
            gate = jnp.dot(norm_ref[...], wg_ref[:, here], preferred_element_type=F32)
            up = jnp.dot(norm_ref[...], wu_ref[:, here], preferred_element_type=F32)
            gate = taps_of(gate, gt_ref[:, here])
            up = taps_of(up, ut_ref[:, here])
            hid_ref[:, here] = (jax.nn.silu(gate) * up).astype(BF)

    whole = lambda shape: pl.BlockSpec(shape, lambda i: (0,) * len(shape))
    return pl.pallas_call(
        body,
        grid=(rows // SEQ,),
        in_specs=[
            smem_spec(),
            smem_spec(),
            pl.BlockSpec((SEQ, dim), lambda i: (i, 0)),
            pl.BlockSpec((SEQ, dim), lambda i: (i, 0)),
            whole((1, dim)),
            whole((3, width)),
            whole((3, width)),
        ]
        + any_specs(2 * n),
        out_specs=[
            pl.BlockSpec((SEQ, width), lambda i: (i, 0)),
            pl.BlockSpec((SEQ, own), lambda i: (i, 0)),
        ],
        out_shape=[jax.ShapeDtypeStruct((rows, width), BF), jax.ShapeDtypeStruct((rows, own), BF)],
        scratch_shapes=[
            pltpu.VMEM((dim, width), BF),
            pltpu.VMEM((dim, width), BF),
            pltpu.VMEM((SEQ, dim), BF),
            pltpu.SemaphoreType.DMA((2,)),
        ],
        compiler_params=pltpu.CompilerParams(dimension_semantics=("arbitrary",)),
        name="feed_forward",
    )(idx, own_at, tokens, mixer_sum, gain, gate_taps, up_taps, *gate_chunks, *up_chunks)


def down(idx, hidden, chunks):
    rows, width = hidden.shape
    cols = chunks[0].shape[1]
    total = cols * (len(chunks) - 1)
    tile = 256

    def body(idx_ref, h_ref, *rest):
        refs, out_ref, (w_ref, sem) = rest[: len(chunks)], rest[len(chunks)], rest[-2:]

        @pl.when(pl.program_id(0) == 0)
        def _():
            todo = copies(list(refs), col_place(idx_ref, w_ref, cols), sem)
            for c in todo:
                c.start()
            for c in todo:
                c.wait()

        for at, size in tiles_of(total, 512):
            here = pl.ds(at, size)
            out_ref[:, here] = jnp.dot(h_ref[...], w_ref[:, here], preferred_element_type=F32).astype(BF)

    return pl.pallas_call(
        body,
        grid=(rows // tile,),
        in_specs=[smem_spec(), pl.BlockSpec((tile, width), lambda i: (i, 0))] + any_specs(len(chunks)),
        out_specs=pl.BlockSpec((tile, total), lambda i: (i, 0)),
        out_shape=jax.ShapeDtypeStruct((rows, total), BF),
        scratch_shapes=[pltpu.VMEM((width, total), BF), pltpu.SemaphoreType.DMA],
        compiler_params=pltpu.CompilerParams(dimension_semantics=("arbitrary",)),
        name="down",
    )(idx, hidden, *chunks)


def per_device(
    ring,
    tokens,
    w_gate_side,
    w_value_side,
    spatial_gain,
    w_spatial,
    spatial_bias,
    w_mixer_out,
    first_gain,
    w_ff_gate,
    w_ff_up,
    conv_gate_taps,
    conv_up_taps,
    w_ff_down,
    second_gain,
):
    rows, dim = tokens.shape
    n_tp = lax.axis_size("tp")
    own = dim // n_tp
    offset = lax.axis_index("tp") * own
    idx = ring.index()
    width = w_value_side.shape[1]

    sides = ring.gather(jnp.concatenate([w_value_side, w_gate_side], axis=1))
    outs = ring.gather(w_mixer_out)
    gates = ring.gather(w_ff_gate)
    ups = ring.gather(w_ff_up)
    cols = w_ff_down.shape[1]
    pieces = max(1, cols // 128)
    size = cols // pieces
    downs = [ring.gather(w_ff_down[:, p * size : (p + 1) * size]) for p in range(pieces)]

    gate_act, value_act = gate_value(idx, tokens, sides, width)
    sums = lax.psum((jnp.sum(value_act, axis=1), jnp.sum(value_act * value_act, axis=1)), "tp")
    mean = sums[0][:, None] / (width * n_tp)
    spread = sums[1][:, None] / (width * n_tp) - mean * mean
    scale = lax.rsqrt(spread + norm_eps)
    part = mixer(
        idx, gate_act, value_act, mean, scale, spatial_gain[None], w_spatial, spatial_bias.T, outs, dim
    )
    mixer_own = lax.psum_scatter(part, "tp", scatter_dimension=1, tiled=True)
    mixer_sum = lax.all_gather(mixer_own, "tp", axis=1, tiled=True)
    hidden, first_own = feed_forward(
        idx,
        offset[None].astype(jnp.int32),
        tokens,
        mixer_sum,
        first_gain[None],
        gates,
        ups,
        conv_gate_taps,
        conv_up_taps,
        own,
    )
    sums = [
        lax.psum_scatter(down(idx, hidden, d), "tp", scatter_dimension=1, tiled=True) for d in downs
    ]
    per = own // cols
    ff_sum = jnp.stack([s.reshape(rows, per, size) for s in sums], axis=2).reshape(rows, own)
    own_gain = lax.dynamic_slice_in_dim(second_gain, offset, own, 0)
    x = residual_scale * first_own.astype(F32) + ff_sum.astype(F32)
    sums = lax.psum((jnp.sum(x, axis=1), jnp.sum(x * x, axis=1)), "tp")
    mean = sums[0][:, None] / dim
    spread = sums[1][:, None] / dim - mean * mean
    return ((x - mean) * lax.rsqrt(spread + norm_eps) * own_gain).astype(BF)


def solution(mesh):
    ring = Ring(cycle_of(mesh))

    def step(*args):
        return per_device(ring, *args)

    return jax.shard_map(
        step,
        mesh=mesh,
        in_specs=(
            P("fs", None),
            P("fs", "tp"),
            P("fs", "tp"),
            P("tp"),
            P("tp", None, None),
            P("tp", None),
            P("tp", "fs"),
            P(),
            P("fs", "tp"),
            P("fs", "tp"),
            P(None, "tp"),
            P(None, "tp"),
            P("tp", "fs"),
            P(),
        ),
        out_specs=P("fs", "tp"),
        check_vma=False,
    )
```
